32 devices in a mesh: ep: 8 (over z, x), tp: 4 (over y, core).
Axes of the slice: x: 2, y: 2, z: 4, core: 2. Of those that a mesh axis runs over, the one named last changes fastest.
Arguments:
- conv_input: bfloat16 [8192, 2048], P('ep', 'tp'), may hold values from -6 to 6
- conv_kernel: bfloat16 [31, 2048], P(None, 'tp'), may hold values from -2 to 2
- norm_gain: float32 [2048], P('tp'), may hold values from 0.1 to 1.9
- norm_shift: float32 [2048], P('tp'), may hold values from -3 to 3
- conv_proj: bfloat16 [2048, 2048], P('tp'), may hold values from -0.125 to 0.125
- moe_input: bfloat16 [2048, 2048], P(('ep', 'tp')), may hold values from -6 to 6
- moe_gain: float32 [2048], replicated, may hold values from 0.1 to 1.9
- routes: int32 [2048, 2], P('ep'), may hold values from 0 to 7, all different within a row; in each aligned block of 256 rows (0 to 255, 256 to 511, ...) at most 128 rows name the same one
- route_weights: float32 [2048, 2], P('ep'), may hold values from 0.2 to 1
- gate_proj: bfloat16 [8, 2048, 2048], P('ep', None, 'tp'), may hold values from -0.125 to 0.125
- up_proj: bfloat16 [8, 2048, 2048], P('ep', None, 'tp'), may hold values from -0.125 to 0.125
- down_proj: bfloat16 [8, 2048, 2048], P('ep', 'tp'), may hold values from -0.125 to 0.125
Outputs:
- conv_out: bfloat16 [8192, 2048], P(('ep', 'tp'))
- moe_out: bfloat16 [2048, 2048], P(('ep', 'tp'))
The draws below stay inside these ranges and needn't reach their ends.
Inputs may be any that keep to these rules, and one draw needn't show every extreme that they name: `routes`: each row names 2 different experts. In each aligned block of 256 rows no expert is named by more than 128 rows, and in some blocks an expert is named by exactly 128 rows.
All inputs are finite; a program needn't handle non-finite values.
Results may differ from the reference program's by a relative error of at most 0.012.
Values may be sent and summed in bfloat16 or wider, within the bound.
A program may use at most 128 MiB of HBM per device.

```python
import math
import jax
import jax.numpy as jnp
import numpy as np
from jax import lax

D = 2048
FE = 2048
CONV_WIDTH = 31
TOPK = 2
TOK_DEV = 64
EXPERTS = 8
CAPG = 128
CONV_TOKENS = 8192
MOE_TOKENS = 2048
N_EP = 8
N_TP = 4


def draw_conv_kernel(key, part):
    first_key, second_key = jax.random.split(jax.random.fold_in(key, 11))
    factors = jax.random.permutation(first_key, jnp.array([0.5, 0.9, 1.6, 2.6], jnp.float32))
    channel_block = jnp.arange(D, dtype=jnp.int32) * 4 // D
    column_scale = factors[channel_block] / math.sqrt(CONV_WIDTH)
    base = jnp.clip(jax.random.normal(second_key, (CONV_WIDTH, D), jnp.float32), -4.0, 4.0)
    return (base * column_scale[None, :]).astype(jnp.bfloat16)


def shard_levels(stream_key, extent, cuts, least, top_value):
    def one(axis_at, parts):
        heights = jax.random.uniform(jax.random.fold_in(jax.random.fold_in(stream_key, 6), axis_at), (parts,), jnp.float32, least / len(cuts), top_value / len(cuts))
        return jnp.repeat(jnp.exp(heights), extent[axis_at] // parts).reshape((-1,) + (1,) * (len(extent) - axis_at - 1))

    factor_of = one(*cuts[0])
    for cut in cuts[1:]:
        factor_of = factor_of * one(*cut)
    return factor_of


def assign_block(own_key, own, number, rows, number_of, top, most, slope):
    ranking = jax.random.permutation(own_key, number_of)
    packed, usual = load_shares(number_of, rows * top, most, slope, True), load_shares(number_of, rows * top, most, slope, False)
    places = jnp.arange(number_of)

    def named(sizes, offset_by):
        used = int((sizes > 0).sum())
        fixed = max(1, used // 4)
        moved = fixed + (places - fixed + offset_by * (used - fixed)) % max(1, number_of - fixed)
        return jnp.zeros((number_of,), jnp.int32).at[ranking[jnp.where(places < fixed, places, moved)]].set(jnp.asarray(sizes, jnp.int32))

    sizes = jnp.where(number % 4 == 0, named(packed, number // 4), named(usual, number - number // 4 - 1))
    mixed = jax.random.permutation(jax.random.fold_in(own, 3), number_of)
    giver, taker = mixed[0:number_of // 2 * 2:2], mixed[1:number_of // 2 * 2:2]
    slack = jnp.minimum(sizes[giver] - 1, most - sizes[taker]) // 2
    slack = jnp.where((giver == ranking[0]) | (taker == ranking[0]) | (sizes[taker] == 0), 0, jnp.maximum(slack, 0))
    moved = jax.random.randint(jax.random.fold_in(own, 4), (number_of // 2,), 0, 1 << 20) % (slack + 1)
    sizes = sizes.at[giver].add(-moved).at[taker].add(moved)
    labels = jnp.searchsorted(jnp.cumsum(sizes), jnp.arange(rows * top), side="right").astype(jnp.int32)
    listing = labels.reshape(top, rows).T
    listing = listing[jax.random.permutation(jax.random.fold_in(own, 1), rows)]
    offset_by = jax.random.randint(jax.random.fold_in(own, 2), (rows, 1), 0, top)
    return jnp.take_along_axis(listing, (jnp.arange(top)[None, :] + offset_by) % top, axis=1)


def load_shares(amount, total, most, slope, full):
    portions = [(1 << 20) // math.isqrt(standing ** slope) + 1 for standing in range(1, amount + 1)]
    largest = most if full else min(most, max(-(-total // amount), total * portions[0] // sum(portions)))
    least = 1 if total - largest >= amount - 1 else 0
    counts, rest = [largest] + [least] * (amount - 1), total - largest - least * (amount - 1)
    while rest > 0:
        candidates = [i for i in range(1, amount) if counts[i] < largest] or [i for i in range(1, amount) if counts[i] < most]
        whole, left = sum([portions[i] for i in candidates]), rest
        for i in candidates:
            more = min(most - counts[i], max(1, left * portions[i] // whole), rest)
            counts[i] = counts[i] + more
            rest = rest - more
    return np.array(counts)


def noise(stream_key, extent, scale, limit, cuts=(), held_as=jnp.bfloat16):
    gain = shard_levels(stream_key, extent, cuts, -0.22, 0.18) if cuts else 1.0
    entries = jax.random.normal(stream_key, extent, jnp.float32) * scale * gain
    return jnp.minimum(jnp.maximum(entries, -limit), limit).astype(held_as)


def setup_inputs(seed: int = 0) -> dict:
    splits = jax.random.split(jax.random.key(seed), 13)
    conv_input = noise(splits[0], (CONV_TOKENS, D), 1.0, 6.0, ((0, 8), (1, 4)))
    conv_kernel = draw_conv_kernel(jax.random.fold_in(splits[12], 71), 0)
    norm_gain = jnp.clip(1.0 + 0.18 * jax.random.normal(splits[2], (D,), jnp.float32), 0.1, 1.9)
    norm_shift = noise(splits[3], (D,), 0.5, 3.0, ((0, 4),), jnp.float32)
    conv_proj = noise(splits[4], (D, D), D ** -0.5, 0.125, ((0, 4),))
    moe_input = noise(splits[5], (MOE_TOKENS, D), 1.0, 6.0, ((0, 32),))
    moe_gain = jnp.clip(1.0 + 0.18 * jax.random.normal(splits[6], (D,), jnp.float32), 0.1, 1.9)
    routes_keys = jax.random.split(jax.random.fold_in(splits[7], 1), MOE_TOKENS // (N_TP * TOK_DEV))
    routes_turns = jax.random.permutation(jax.random.fold_in(splits[7], 3), MOE_TOKENS // (N_TP * TOK_DEV))
    routes = jax.vmap(lambda own, number: assign_block(jax.random.fold_in(splits[7], 2), own, number, N_TP * TOK_DEV, EXPERTS, TOPK, CAPG, 2))(routes_keys, routes_turns).reshape((MOE_TOKENS, TOPK))
    route_weights = jnp.clip(0.2 + 0.8 * jax.random.uniform(splits[8], (MOE_TOKENS, TOPK), jnp.float32) ** shard_levels(splits[8], (MOE_TOKENS, TOPK), ((0, 8),), -0.2, 0.2), 0.2, 1.0)
    gate_proj = noise(splits[9], (EXPERTS, D, FE), D ** -0.5, 0.125, ((0, 8), (2, 4)))
    up_proj = noise(splits[10], (EXPERTS, D, FE), D ** -0.5, 0.125, ((0, 8), (2, 4)))
    down_proj = noise(splits[11], (EXPERTS, FE, D), FE ** -0.5, 0.125, ((0, 8), (1, 4)))
    return dict(conv_input=conv_input, conv_kernel=conv_kernel, norm_gain=norm_gain, norm_shift=norm_shift, conv_proj=conv_proj, moe_input=moe_input, moe_gain=moe_gain, routes=routes, route_weights=route_weights, gate_proj=gate_proj, up_proj=up_proj, down_proj=down_proj)


def conv_half(conv_input, conv_kernel, norm_gain, norm_shift, conv_proj):
    reach = CONV_WIDTH - 1
    padded = jnp.concatenate([jnp.zeros((reach, D), conv_input.dtype), conv_input], axis=0)
    taps = conv_kernel.astype(jnp.float32)
    mixed = jnp.zeros((CONV_TOKENS, D), jnp.float32)
    for offset in range(CONV_WIDTH):
        mixed = mixed + padded[offset:offset + CONV_TOKENS].astype(jnp.float32) * taps[offset]
    center = lax.optimization_barrier(jnp.sum(mixed, axis=1)) / D
    spread = jnp.maximum(lax.optimization_barrier(jnp.sum(mixed * mixed, axis=1)) / D - center * center, 0.0)
    scaled = (mixed - center[:, None]) * lax.rsqrt(spread[:, None] + 1e-05) * norm_gain + norm_shift
    activated = jax.nn.silu(scaled).astype(jnp.bfloat16)
    block = D // N_TP
    total = jnp.zeros((CONV_TOKENS, D), jnp.float32)
    for part in range(N_TP):
        piece = jnp.dot(activated[:, part * block:(part + 1) * block], conv_proj[part * block:(part + 1) * block], preferred_element_type=jnp.float32)
        total = total + lax.optimization_barrier(piece.astype(jnp.bfloat16)).astype(jnp.float32)
    return total.astype(jnp.bfloat16)

def moe_half(moe_input, moe_gain, routes, route_weights, gate_proj, up_proj, down_proj):
    moe_float = moe_input.astype(jnp.float32)
    normed = (moe_float * lax.rsqrt(lax.optimization_barrier(jnp.mean(moe_float * moe_float, axis=1, keepdims=True)) + 1e-06) * moe_gain).astype(jnp.bfloat16)
    block = FE // N_TP
    slots = N_EP * CAPG

    def one_expert(total, items):
        expert, gate_w, up_w, down_w = items
        hits = routes == expert
        weight = lax.optimization_barrier(jnp.sum(jnp.where(hits, route_weights, 0.0), axis=1))
        named = jnp.any(hits, axis=1)
        index = jnp.nonzero(named, size=slots, fill_value=0)[0].astype(jnp.int32)
        valid = jnp.arange(slots, dtype=jnp.int32) < jnp.sum(named.astype(jnp.int32))
        rows = normed[index]
        result = jnp.zeros((slots, D), jnp.float32)
        for part in range(N_TP):
            low = part * block
            gated = jax.nn.silu(jnp.dot(rows, gate_w[:, low:low + block], preferred_element_type=jnp.float32))
            hidden = (gated * jnp.dot(rows, up_w[:, low:low + block], preferred_element_type=jnp.float32)).astype(jnp.bfloat16)
            piece = jnp.dot(hidden, down_w[low:low + block], preferred_element_type=jnp.float32)
            result = result + lax.optimization_barrier(piece.astype(jnp.bfloat16)).astype(jnp.float32)
        scale = jnp.where(valid, weight[index], 0.0)
        return (total.at[index].add(result * scale[:, None]), None)
    experts = jnp.arange(EXPERTS, dtype=jnp.int32)
    total, _ = lax.scan(one_expert, jnp.zeros((MOE_TOKENS, D), jnp.float32), (experts, gate_proj, up_proj, down_proj))
    return total.astype(jnp.bfloat16)

def reference(conv_input, conv_kernel, norm_gain, norm_shift, conv_proj, moe_input, moe_gain, routes, route_weights, gate_proj, up_proj, down_proj):
    conv_out = conv_half(conv_input, conv_kernel, norm_gain, norm_shift, conv_proj)
    moe_out = moe_half(moe_input, moe_gain, routes, route_weights, gate_proj, up_proj, down_proj)
    return (conv_out, moe_out)
```

```python
import jax
import jax.numpy as jnp
from jax import lax
from jax.sharding import PartitionSpec as P


def shifted(value, axis, steps):
    count = lax.axis_size(axis)
    leading, last = (max(0, -steps), min(count, count - steps))
    return lax.ppermute(value, axis, [(source, source + steps) for source in range(leading, last)])


def local(
    conv_input,
    conv_kernel,
    norm_gain,
    norm_shift,
    conv_proj,
    moe_input,
    moe_gain,
    routes,
    route_weights,
    gate_proj,
    up_proj,
    down_proj,
):
    tp_count = lax.axis_size("tp")
    ep_count = lax.axis_size("ep")
    local_rows, local_width = conv_input.shape
    reach = conv_kernel.shape[0] - 1
    history = shifted(conv_input[local_rows - reach :], "ep", 1)
    padded = jnp.concatenate([history, conv_input], axis=0)
    taps = conv_kernel.astype(jnp.float32)
    mixed = jnp.zeros((local_rows, local_width), jnp.float32)
    for offset in range(reach + 1):
        mixed = mixed + padded[offset : offset + local_rows].astype(jnp.float32) * taps[offset]
    full_width = local_width * tp_count
    sums, squares = lax.psum((jnp.sum(mixed, axis=1), jnp.sum(mixed * mixed, axis=1)), "tp")
    center = sums / full_width
    spread = jnp.maximum(squares / full_width - center * center, 0.0)
    scaled = (mixed - center[:, None]) * lax.rsqrt(spread[:, None] + 1e-05) * norm_gain + norm_shift
    activated = jax.nn.silu(scaled).astype(jnp.bfloat16)
    conv_out = lax.psum_scatter(
        jnp.dot(activated, conv_proj, preferred_element_type=jnp.float32).astype(jnp.bfloat16),
        "tp",
        scatter_dimension=0,
        tiled=True,
    )
    moe_float = moe_input.astype(jnp.float32)
    normed = (
        moe_float
        * lax.rsqrt(jnp.mean(moe_float * moe_float, axis=1, keepdims=True) + 1e-06)
        * moe_gain
    ).astype(jnp.bfloat16)
    group = lax.all_gather(normed, "tp", axis=0, tiled=True)
    group_rows, top_count = routes.shape
    model_width = group.shape[1]
    capacity = 2 * top_count * group_rows // ep_count
    share = capacity // tp_count
    experts = jnp.arange(ep_count, dtype=jnp.int32)
    named = routes.T[None, :, :] == experts[:, None, None]
    hit = jnp.any(named, axis=1)
    weight = jnp.sum(jnp.where(named, route_weights.T[None, :, :], 0.0), axis=1)
    tokens = jnp.arange(group_rows, dtype=jnp.int32)
    before = (tokens[:, None] < tokens[None, :]).astype(jnp.bfloat16)
    rank = jnp.dot(hit.astype(jnp.bfloat16), before, preferred_element_type=jnp.float32).astype(
        jnp.int32
    )
    first = lax.axis_index("tp") * share
    slots = first + jnp.arange(share, dtype=jnp.int32)
    held = hit[:, None, :] & (rank[:, None, :] == slots[None, :, None])
    pick = held.astype(jnp.bfloat16).reshape(ep_count * share, group_rows)
    scale = (
        jnp.where(held, weight[:, None, :], 0.0)
        .astype(jnp.bfloat16)
        .reshape(ep_count * share, group_rows)
    )
    outgoing = jnp.dot(pick, group, preferred_element_type=jnp.float32).astype(jnp.bfloat16)
    landed = lax.all_to_all(
        outgoing.reshape(ep_count, share, model_width), "ep", split_axis=0, concat_axis=0, tiled=True
    ).reshape(ep_count * share, model_width)
    incoming = lax.all_gather(landed, "tp", axis=0, tiled=True)
    gated = jax.nn.silu(jnp.dot(incoming, gate_proj[0], preferred_element_type=jnp.float32))
    hidden = (gated * jnp.dot(incoming, up_proj[0], preferred_element_type=jnp.float32)).astype(
        jnp.bfloat16
    )
    pieces = jnp.dot(hidden, down_proj[0], preferred_element_type=jnp.float32).astype(jnp.bfloat16)
    summed = lax.psum_scatter(pieces, "tp", scatter_dimension=0, tiled=True)
    returned = lax.all_to_all(
        summed.reshape(ep_count, share, model_width), "ep", split_axis=0, concat_axis=0, tiled=True
    ).reshape(ep_count * share, model_width)
    combined = lax.dot_general(
        scale, returned, (((0,), (0,)), ((), ())), preferred_element_type=jnp.float32
    )
    moe_out = lax.psum_scatter(combined.astype(jnp.bfloat16), "tp", scatter_dimension=0, tiled=True)
    return (conv_out, moe_out)


def solution(mesh):
    placed = (
        P("ep", "tp"),
        P(None, "tp"),
        P("tp"),
        P("tp"),
        P("tp", None),
        P(("ep", "tp"), None),
        P(),
        P("ep", None),
        P("ep", None),
        P("ep", None, "tp"),
        P("ep", None, "tp"),
        P("ep", "tp", None),
    )
    return jax.shard_map(
        local,
        mesh=mesh,
        in_specs=placed,
        out_specs=(P(("ep", "tp"), None), P(("ep", "tp"), None)),
        check_vma=False,
    )
```

```python
import functools

import jax
import jax.numpy as jnp
from jax import lax
from jax.experimental import pallas as pl
from jax.experimental.pallas import tpu as pltpu
from jax.sharding import PartitionSpec as P

MESH = pl.DeviceIdType.MESH


def hop_order(ep_count):
    half = ep_count // 2
    order = [0, half]
    for near in range(1, half):
        order += [half - near, half + near]
    return order


def exchange(
    normed, pick, scale, partial, gate_hbm, up_hbm, down_hbm,
    conv_out, moe_out,
    gate, up, down, group, outgoing, arrived, pieces, from_core, to_y, from_y, to_ep, returned,
    conv_core, conv_to_y, conv_from_y, combined, last_core, last_to_y, last_from_y,
    weight_sem, ag_send, ag_recv, ep_send, ep_recv, fan_send, fan_recv,
    core_send, core_recv, y_send, y_recv, back_send, back_recv,
    conv_send, conv_recv, last_send, last_recv,
    *, ep_count, share,
):
    order = hop_order(ep_count)
    me_ep, me = lax.axis_index("ep"), lax.axis_index("tp")
    core = me + 1 - 2 * (me % 2)
    over = (me + 2) % 4
    far = (core + 2) % 4
    rows, width = normed.shape
    f32, bf16 = jnp.float32, jnp.bfloat16

    def remote(src, dst, send, recv, where):
        return pltpu.make_async_remote_copy(
            src_ref=src, dst_ref=dst, send_sem=send, recv_sem=recv, device_id=where,
            device_id_type=MESH,
        )

    def block(ref, index, size):
        return ref.at[pl.ds(pl.multiple_of(index * size, size), size)]

    loads = [
        pltpu.make_async_copy(src, dst, weight_sem.at[i])
        for i, (src, dst) in enumerate(((gate_hbm, gate), (up_hbm, up), (down_hbm, down)))
    ]
    for load in loads:
        load.start()
    barrier = pltpu.get_barrier_semaphore()
    pl.semaphore_signal(barrier, inc=1, device_id={"tp": core}, device_id_type=MESH)
    pl.semaphore_signal(barrier, inc=1, device_id={"tp": over}, device_id_type=MESH)
    for d in range(1, ep_count):
        pl.semaphore_signal(
            barrier, inc=1, device_id={"ep": (me_ep + d) % ep_count}, device_id_type=MESH
        )
    pl.semaphore_wait(barrier, ep_count + 1)

    sent = []

    ag = [
        remote(normed, block(group, me, rows), ag_send.at[0], ag_recv.at[0], {"tp": over}),
        remote(normed, block(group, me, rows), ag_send.at[1], ag_recv.at[1], {"tp": core}),
        remote(block(group, over, rows), block(group, over, rows), ag_send.at[2], ag_recv.at[2], {"tp": core}),
    ]
    ag[0].start()
    ag[1].start()
    group[pl.ds(pl.multiple_of(me * rows, rows), rows), :] = normed[...]
    span = partial.shape[0] // 4
    conv = [
        remote(
            block(partial, core if n == 0 else far, span), conv_core.at[n],
            conv_send.at[n], conv_recv.at[n], {"tp": core},
        )
        for n in range(2)
    ]
    ag[0].wait_recv()
    ag[2].start()
    conv[1].start()
    conv[0].start()
    ag[1].wait_recv()
    ag[2].wait_recv()
    sent += ag + conv

    tile = 512
    for n in range(0, width, tile):
        part = jnp.dot(pick[...], group[:, n : n + tile], preferred_element_type=f32).astype(bf16)
        outgoing[:, n : n + tile] = part
        arrived[pl.ds(pl.multiple_of(me * share, share), share), n : n + tile] = part[:share]
    ep = []
    for s in range(1, ep_count):
        ep.append(
            remote(
                outgoing.at[s * share : (s + 1) * share], block(arrived, s * 4 + me, share),
                ep_send.at[s], ep_recv.at[s], {"ep": (me_ep + order[s]) % ep_count},
            )
        )
        ep[-1].start()
    sent += ep

    def fan(kind, s):
        quarter = over if kind == 2 else me
        place = block(arrived, s * 4 + quarter, share)
        return remote(
            place, place, fan_send.at[kind, s], fan_recv.at[kind, s],
            {"tp": over if kind == 0 else core},
        )

    fans = [[fan(kind, s) for s in range(ep_count)] for kind in range(3)]
    for kind in range(3):
        sent += fans[kind]

    def relay(s):
        fans[0][s].wait_recv()
        fans[2][s].start()

    def land(s):
        if s > 0:
            ep[s - 1].wait_recv()
        fans[0][s].start()
        fans[1][s].start()

    conv_y = [
        remote(conv_to_y.at[n], conv_from_y.at[n], conv_send.at[2 + n], conv_recv.at[2 + n], {"tp": over})
        for n in range(4)
    ]
    sent += conv_y
    piece_rows = span // 4

    def conv_half():
        conv[1].wait_recv()
        for n in range(4):
            at = pl.multiple_of(over * span + n * piece_rows, piece_rows)
            conv_to_y[n] = (
                partial[pl.ds(at, piece_rows), :].astype(f32)
                + conv_core[1, n * piece_rows : (n + 1) * piece_rows, :].astype(f32)
            ).astype(bf16)
            conv_y[n].start()

    chunk = 2 * 4 * share

    def experts(c):
        for s in (2 * c, 2 * c + 1):
            fans[1][s].wait_recv()
            fans[2][s].wait_recv()
        here = slice(c * chunk, (c + 1) * chunk)
        lines = arrived[here, :]
        left = jnp.dot(lines, gate[...], preferred_element_type=f32)
        right = jnp.dot(lines, up[...], preferred_element_type=f32)
        hidden = (left / (1.0 + jnp.exp(-left)) * right).astype(bf16)
        for n in range(0, width, tile):
            pieces[here, n : n + tile] = jnp.dot(
                hidden, down[:, n : n + tile], preferred_element_type=f32
            ).astype(bf16)
        for s in (2 * c, 2 * c + 1):
            cores[s][1].start()
            cores[s][0].start()

    cores = [
        [
            remote(
                block(pieces, s * 4 + (core if n == 0 else far), share), from_core.at[s, n],
                core_send.at[s, n], core_recv.at[s, n], {"tp": core},
            )
            for n in range(2)
        ]
        for s in range(ep_count)
    ]
    ys = [
        remote(to_y.at[s], from_y.at[s], y_send.at[s], y_recv.at[s], {"tp": over})
        for s in range(ep_count)
    ]
    backs = [
        remote(
            to_ep.at[s], returned.at[s * share : (s + 1) * share], back_send.at[s], back_recv.at[s],
            {"ep": (me_ep + ep_count - order[s]) % ep_count},
        )
        for s in range(1, ep_count)
    ]
    for s in range(ep_count):
        sent += cores[s]
    sent += ys + backs

    def mine(s, quarter, n):
        at = pl.multiple_of((s * 4 + quarter) * share, share)
        return pieces[pl.ds(at, share), :].astype(f32) + from_core[s, n].astype(f32)

    def across(c):
        for s in (2 * c, 2 * c + 1):
            cores[s][1].wait_recv()
            to_y[s] = mine(s, over, 1).astype(bf16)
            ys[s].start()

    def back(c):
        for s in (2 * c, 2 * c + 1):
            cores[s][0].wait_recv()
            ys[s].wait_recv()
            total = (mine(s, me, 0) + from_y[s].astype(f32)).astype(bf16)
            if s == 0:
                returned[:share, :] = total
            else:
                to_ep[s] = total
                backs[s - 1].start()

    chunks = ep_count // 2
    land(0)
    for s in range(1, ep_count):
        land(s)
        if s >= 2:
            relay(s - 2)
        if s == 3:
            for load in loads:
                load.wait()
        if s == 5:
            experts(0)
    experts(1)
    across(0)
    relay(ep_count - 2)
    relay(ep_count - 1)
    conv_half()
    for c in range(2, chunks):
        experts(c)
        across(c - 1)
        back(c - 2)
    across(chunks - 1)
    back(chunks - 2)
    conv[0].wait_recv()
    for n in range(4):
        conv_y[n].wait_recv()
        at = pl.multiple_of(me * span + n * piece_rows, piece_rows)
        conv_out[n * piece_rows : (n + 1) * piece_rows, :] = (
            partial[pl.ds(at, piece_rows), :].astype(f32)
            + conv_core[0, n * piece_rows : (n + 1) * piece_rows, :].astype(f32)
            + conv_from_y[n].astype(f32)
        ).astype(bf16)
    back(chunks - 1)

    for r in backs:
        r.wait_recv()
    for n in range(0, width, tile):
        combined[:, n : n + tile] = jnp.dot(
            scale[...], returned[:, n : n + tile], preferred_element_type=f32
        ).astype(bf16)
    last = [
        remote(
            block(combined, core if n == 0 else far, rows), last_core.at[n],
            last_send.at[n], last_recv.at[n], {"tp": core},
        )
        for n in range(2)
    ]
    last[1].start()
    last[0].start()
    last.append(remote(last_to_y, last_from_y, last_send.at[2], last_recv.at[2], {"tp": over}))

    def own(quarter, n):
        at = pl.multiple_of(quarter * rows, rows)
        return combined[pl.ds(at, rows), :].astype(f32) + last_core[n].astype(f32)

    last[1].wait_recv()
    last_to_y[...] = own(over, 1).astype(bf16)
    last[2].start()
    last[0].wait_recv()
    last[2].wait_recv()
    moe_out[...] = (own(me, 0) + last_from_y[...].astype(f32)).astype(bf16)
    sent += last
    for r in sent:
        r.wait_send()


def run_exchange(normed, pick, scale, partial, gate, up, down, ep_count, share):
    rows, width = normed.shape
    hid = gate.shape[1]
    span = partial.shape[0] // 4
    bf16 = jnp.bfloat16
    slots = ep_count * share
    vmem, dma = pltpu.VMEM, pltpu.SemaphoreType.DMA
    at_vmem, at_any = pl.BlockSpec(memory_space=pltpu.VMEM), pl.BlockSpec(memory_space=pl.ANY)
    return pl.pallas_call(
        functools.partial(exchange, ep_count=ep_count, share=share),
        out_shape=(
            jax.ShapeDtypeStruct((span, width), bf16),
            jax.ShapeDtypeStruct((rows, width), bf16),
        ),
        in_specs=[at_vmem] * 4 + [at_any] * 3,
        out_specs=(at_vmem, at_vmem),
        scratch_shapes=[
            vmem((width, hid), bf16),
            vmem((width, hid), bf16),
            vmem((hid, width), bf16),
            vmem((4 * rows, width), bf16),
            vmem((slots, width), bf16),
            vmem((4 * slots, width), bf16),
            vmem((4 * slots, width), bf16),
            vmem((ep_count, 2, share, width), bf16),
            vmem((ep_count, share, width), bf16),
            vmem((ep_count, share, width), bf16),
            vmem((ep_count, share, width), bf16),
            vmem((slots, width), bf16),
            vmem((2, span, width), bf16),
            vmem((4, span // 4, width), bf16),
            vmem((4, span // 4, width), bf16),
            vmem((4 * rows, width), bf16),
            vmem((2, rows, width), bf16),
            vmem((rows, width), bf16),
            vmem((rows, width), bf16),
            dma((3,)),
            dma((3,)), dma((3,)),
            dma((ep_count,)), dma((ep_count,)),
            dma((3, ep_count)), dma((3, ep_count)),
            dma((ep_count, 2)), dma((ep_count, 2)),
            dma((ep_count,)), dma((ep_count,)),
            dma((ep_count,)), dma((ep_count,)),
            dma((6,)), dma((6,)),
            dma((3,)), dma((3,)),
        ],
        compiler_params=pltpu.CompilerParams(
            collective_id=0, has_side_effects=True, vmem_limit_bytes=60 * 1024 * 1024
        ),
    )(normed, pick, scale, partial, gate, up, down)


def shifted(value, axis, steps):
    count = lax.axis_size(axis)
    leading, last = (max(0, -steps), min(count, count - steps))
    return lax.ppermute(value, axis, [(source, source + steps) for source in range(leading, last)])


def local(
    conv_input,
    conv_kernel,
    norm_gain,
    norm_shift,
    conv_proj,
    moe_input,
    moe_gain,
    routes,
    route_weights,
    gate_proj,
    up_proj,
    down_proj,
):
    tp_count = lax.axis_size("tp")
    ep_count = lax.axis_size("ep")
    local_rows, local_width = conv_input.shape
    reach = conv_kernel.shape[0] - 1
    history = shifted(conv_input[local_rows - reach :], "ep", 1)
    padded = jnp.concatenate([history, conv_input], axis=0)
    taps = conv_kernel.astype(jnp.float32)
    mixed = jnp.zeros((local_rows, local_width), jnp.float32)
    for offset in range(reach + 1):
        mixed = mixed + padded[offset : offset + local_rows].astype(jnp.float32) * taps[offset]
    full_width = local_width * tp_count
    sums, squares = lax.psum((jnp.sum(mixed, axis=1), jnp.sum(mixed * mixed, axis=1)), "tp")
    center = sums / full_width
    spread = jnp.maximum(squares / full_width - center * center, 0.0)
    scaled = (mixed - center[:, None]) * lax.rsqrt(spread[:, None] + 1e-05) * norm_gain + norm_shift
    activated = jax.nn.silu(scaled).astype(jnp.bfloat16)
    partial = jnp.dot(activated, conv_proj, preferred_element_type=jnp.float32).astype(jnp.bfloat16)
    moe_float = moe_input.astype(jnp.float32)
    normed = (
        moe_float
        * lax.rsqrt(jnp.mean(moe_float * moe_float, axis=1, keepdims=True) + 1e-06)
        * moe_gain
    ).astype(jnp.bfloat16)
    group_rows, top_count = routes.shape
    model_width = normed.shape[1]
    capacity = 2 * top_count * group_rows // ep_count
    share = capacity // tp_count
    direct = tp_count == 4 and share % 16 == 0 and ep_count % 2 == 0 and ep_count >= 8
    if direct:
        hops = jnp.array(hop_order(ep_count), jnp.int32)
        experts = (lax.axis_index("ep") + hops) % ep_count
    else:
        experts = jnp.arange(ep_count, dtype=jnp.int32)
    named = routes.T[None, :, :] == experts[:, None, None]
    hit = jnp.any(named, axis=1)
    weight = jnp.sum(jnp.where(named, route_weights.T[None, :, :], 0.0), axis=1)
    tokens = jnp.arange(group_rows, dtype=jnp.int32)
    before = (tokens[:, None] < tokens[None, :]).astype(jnp.bfloat16)
    rank = jnp.dot(hit.astype(jnp.bfloat16), before, preferred_element_type=jnp.float32).astype(
        jnp.int32
    )
    first = lax.axis_index("tp") * share
    slots = first + jnp.arange(share, dtype=jnp.int32)
    held = hit[:, None, :] & (rank[:, None, :] == slots[None, :, None])
    pick = held.astype(jnp.bfloat16).reshape(ep_count * share, group_rows)
    scale = (
        jnp.where(held, weight[:, None, :], 0.0)
        .astype(jnp.bfloat16)
        .reshape(ep_count * share, group_rows)
    )
    if direct:
        return run_exchange(
            normed, pick, scale.T, partial, gate_proj[0], up_proj[0], down_proj[0], ep_count, share
        )
    conv_out = lax.psum_scatter(partial, "tp", scatter_dimension=0, tiled=True)
    group = lax.all_gather(normed, "tp", axis=0, tiled=True)
    outgoing = jnp.dot(pick, group, preferred_element_type=jnp.float32).astype(jnp.bfloat16)
    landed = lax.all_to_all(
        outgoing.reshape(ep_count, share, model_width), "ep", split_axis=0, concat_axis=0, tiled=True
    ).reshape(ep_count * share, model_width)
    incoming = lax.all_gather(landed, "tp", axis=0, tiled=True)
    gated = jax.nn.silu(jnp.dot(incoming, gate_proj[0], preferred_element_type=jnp.float32))
    hidden = (gated * jnp.dot(incoming, up_proj[0], preferred_element_type=jnp.float32)).astype(
        jnp.bfloat16
    )
    pieces = jnp.dot(hidden, down_proj[0], preferred_element_type=jnp.float32).astype(jnp.bfloat16)
    summed = lax.psum_scatter(pieces, "tp", scatter_dimension=0, tiled=True)
    returned = lax.all_to_all(
        summed.reshape(ep_count, share, model_width), "ep", split_axis=0, concat_axis=0, tiled=True
    ).reshape(ep_count * share, model_width)
    combined = lax.dot_general(
        scale, returned, (((0,), (0,)), ((), ())), preferred_element_type=jnp.float32
    )
    moe_out = lax.psum_scatter(combined.astype(jnp.bfloat16), "tp", scatter_dimension=0, tiled=True)
    return (conv_out, moe_out)


def solution(mesh):
    placed = (
        P("ep", "tp"),
        P(None, "tp"),
        P("tp"),
        P("tp"),
        P("tp", None),
        P(("ep", "tp"), None),
        P(),
        P("ep", None),
        P("ep", None),
        P("ep", None, "tp"),
        P("ep", None, "tp"),
        P("ep", "tp", None),
    )
    return jax.shard_map(
        local,
        mesh=mesh,
        in_specs=placed,
        out_specs=(P(("ep", "tp"), None), P(("ep", "tp"), None)),
        check_vma=False,
    )
```

```python
import functools

import jax
import jax.numpy as jnp
from jax import lax
from jax.experimental import pallas as pl
from jax.experimental.pallas import tpu as pltpu
from jax.sharding import PartitionSpec as P

MESH = pl.DeviceIdType.MESH


def hop_order(ep_count):
    half = ep_count // 2
    order = [0, half]
    for near in range(1, half):
        order += [half - near, half + near]
    return order


def exchange(
    normed, ranks, weights, mixed, stats, gain, shift, proj, gate_hbm, up_hbm, down_hbm,
    conv_out, moe_out,
    partial, stats_in, columns, gate, up, down, group, outgoing, arrived, pieces, from_core, to_y, from_y, to_ep, returned,
    conv_core, conv_to_y, conv_from_y, combined, last_core, last_to_y, last_from_y,
    weight_sem, stats_send, stats_recv, ag_send, ag_recv, ep_send, ep_recv, fan_send, fan_recv,
    core_send, core_recv, y_send, y_recv, back_send, back_recv,
    conv_send, conv_recv, last_send, last_recv,
    *, ep_count, share,
):
    order = hop_order(ep_count)
    me_ep, me = lax.axis_index("ep"), lax.axis_index("tp")
    core = me + 1 - 2 * (me % 2)
    over = (me + 2) % 4
    far = (core + 2) % 4
    rows, width = normed.shape
    f32, bf16 = jnp.float32, jnp.bfloat16

    def remote(src, dst, send, recv, where):
        return pltpu.make_async_remote_copy(
            src_ref=src, dst_ref=dst, send_sem=send, recv_sem=recv, device_id=where,
            device_id_type=MESH,
        )

    def block(ref, index, size):
        return ref.at[pl.ds(pl.multiple_of(index * size, size), size)]

    loads = [
        pltpu.make_async_copy(src, dst, weight_sem.at[i])
        for i, (src, dst) in enumerate(((gate_hbm, gate), (up_hbm, up), (down_hbm, down)))
    ]
    for load in loads:
        load.start()
    barrier = pltpu.get_barrier_semaphore()
    pl.semaphore_signal(barrier, inc=1, device_id={"tp": core}, device_id_type=MESH)
    pl.semaphore_signal(barrier, inc=1, device_id={"tp": over}, device_id_type=MESH)
    pl.semaphore_signal(barrier, inc=1, device_id={"tp": far}, device_id_type=MESH)
    for d in range(1, ep_count):
        pl.semaphore_signal(
            barrier, inc=1, device_id={"ep": (me_ep + d) % ep_count}, device_id_type=MESH
        )
    pl.semaphore_wait(barrier, ep_count + 2)

    sent = []

    ag = [
        remote(normed, block(group, me, rows), ag_send.at[0], ag_recv.at[0], {"tp": over}),
        remote(normed, block(group, me, rows), ag_send.at[1], ag_recv.at[1], {"tp": core}),
        remote(block(group, over, rows), block(group, over, rows), ag_send.at[2], ag_recv.at[2], {"tp": core}),
    ]
    moments = [
        remote(stats, stats_in.at[n], stats_send.at[n], stats_recv.at[n], {"tp": where})
        for n, where in enumerate((over, core, far))
    ]
    sent += moments
    ag[0].start()
    ag[1].start()
    for r in moments:
        r.start()
    group[pl.ds(pl.multiple_of(me * rows, rows), rows), :] = normed[...]
    span = partial.shape[0] // 4
    conv = [
        remote(
            block(partial, core if n == 0 else far, span), conv_core.at[n],
            conv_send.at[n], conv_recv.at[n], {"tp": core},
        )
        for n in range(2)
    ]
    ag[0].wait_recv()
    ag[2].start()
    ag[1].wait_recv()
    ag[2].wait_recv()
    sent += ag + conv

    tile = 512
    group_rows = ranks.shape[1]
    wanted = me * share + lax.broadcasted_iota(jnp.int32, (share, group_rows), 0)
    held = [ranks[s : s + 1, :] == wanted for s in range(ep_count)]
    pick = jnp.concatenate([jnp.where(h, 1.0, 0.0) for h in held], axis=0).astype(bf16)
    for n in range(0, width, tile):
        part = jnp.dot(pick, group[:, n : n + tile], preferred_element_type=f32).astype(bf16)
        outgoing[:, n : n + tile] = part
        arrived[pl.ds(pl.multiple_of(me * share, share), share), n : n + tile] = part[:share]
    ep = []
    for s in range(1, ep_count):
        ep.append(
            remote(
                outgoing.at[s * share : (s + 1) * share], block(arrived, s * 4 + me, share),
                ep_send.at[s], ep_recv.at[s], {"ep": (me_ep + order[s]) % ep_count},
            )
        )
        ep[-1].start()
    sent += ep

    def center_and_scale():
        for r in moments:
            r.wait_recv()
        total = (stats[...] + stats_in[0] + stats_in[1] + stats_in[2]) / width
        center = total[0:1, :]
        spread = jnp.maximum(total[1:2, :] - center * center, 0.0)
        both = jnp.concatenate([center, lax.rsqrt(spread + 1e-05)] + [center] * 6, axis=0)
        columns[...] = both.T

    def project(quarter):
        at = pl.multiple_of(quarter * span, span)
        view = pl.ds(at, span)
        col = columns[view, :]
        scaled = (mixed[view, :] - col[:, 0:1]) * col[:, 1:2] * gain[...] + shift[...]
        activated = (scaled / (1.0 + jnp.exp(-scaled))).astype(bf16)
        for n in range(0, width, tile):
            partial[view, n : n + tile] = jnp.dot(
                activated, proj[:, n : n + tile], preferred_element_type=f32
            ).astype(bf16)

    def fan(kind, s):
        quarter = over if kind == 2 else me
        place = block(arrived, s * 4 + quarter, share)
        return remote(
            place, place, fan_send.at[kind, s], fan_recv.at[kind, s],
            {"tp": over if kind == 0 else core},
        )

    fans = [[fan(kind, s) for s in range(ep_count)] for kind in range(3)]
    for kind in range(3):
        sent += fans[kind]

    def relay(s):
        fans[0][s].wait_recv()
        fans[2][s].start()

    def land(s):
        if s > 0:
            ep[s - 1].wait_recv()
        fans[0][s].start()
        fans[1][s].start()

    conv_y = [
        remote(conv_to_y.at[n], conv_from_y.at[n], conv_send.at[2 + n], conv_recv.at[2 + n], {"tp": over})
        for n in range(4)
    ]
    sent += conv_y
    piece_rows = span // 4

    def conv_half():
        conv[1].wait_recv()
        for n in range(4):
            at = pl.multiple_of(over * span + n * piece_rows, piece_rows)
            conv_to_y[n] = (
                partial[pl.ds(at, piece_rows), :].astype(f32)
                + conv_core[1, n * piece_rows : (n + 1) * piece_rows, :].astype(f32)
            ).astype(bf16)
            conv_y[n].start()

    chunk = 2 * 4 * share

    def experts(c):
        for s in (2 * c, 2 * c + 1):
            fans[1][s].wait_recv()
            fans[2][s].wait_recv()
        here = slice(c * chunk, (c + 1) * chunk)
        lines = arrived[here, :]
        left = jnp.dot(lines, gate[...], preferred_element_type=f32)
        right = jnp.dot(lines, up[...], preferred_element_type=f32)
        hidden = (left / (1.0 + jnp.exp(-left)) * right).astype(bf16)
        for n in range(0, width, tile):
            pieces[here, n : n + tile] = jnp.dot(
                hidden, down[:, n : n + tile], preferred_element_type=f32
            ).astype(bf16)
        for s in (2 * c, 2 * c + 1):
            cores[s][1].start()
            cores[s][0].start()

    cores = [
        [
            remote(
                block(pieces, s * 4 + (core if n == 0 else far), share), from_core.at[s, n],
                core_send.at[s, n], core_recv.at[s, n], {"tp": core},
            )
            for n in range(2)
        ]
        for s in range(ep_count)
    ]
    ys = [
        remote(to_y.at[s], from_y.at[s], y_send.at[s], y_recv.at[s], {"tp": over})
        for s in range(ep_count)
    ]
    backs = [
        remote(
            to_ep.at[s], returned.at[s * share : (s + 1) * share], back_send.at[s], back_recv.at[s],
            {"ep": (me_ep + ep_count - order[s]) % ep_count},
        )
        for s in range(1, ep_count)
    ]
    for s in range(ep_count):
        sent += cores[s]
    sent += ys + backs

    def mine(s, quarter, n):
        at = pl.multiple_of((s * 4 + quarter) * share, share)
        return pieces[pl.ds(at, share), :].astype(f32) + from_core[s, n].astype(f32)

    def across(c):
        for s in (2 * c, 2 * c + 1):
            cores[s][1].wait_recv()
            to_y[s] = mine(s, over, 1).astype(bf16)
            ys[s].start()

    def back(c):
        for s in (2 * c, 2 * c + 1):
            cores[s][0].wait_recv()
            ys[s].wait_recv()
            total = (mine(s, me, 0) + from_y[s].astype(f32)).astype(bf16)
            if s == 0:
                returned[:share, :] = total
            else:
                to_ep[s] = total
                backs[s - 1].start()

    chunks = ep_count // 2
    land(0)
    for s in range(1, ep_count):
        land(s)
        if s >= 2:
            relay(s - 2)
        if s == 1:
            center_and_scale()
            project(far)
            conv[1].start()
        if s == 2:
            project(core)
            conv[0].start()
        if s == 3:
            project(over)
        if s == 4:
            project(me)
        if s == 3:
            for load in loads:
                load.wait()
        if s == 5:
            experts(0)
    experts(1)
    across(0)
    relay(ep_count - 2)
    relay(ep_count - 1)
    conv_half()
    for c in range(2, chunks):
        experts(c)
        across(c - 1)
        back(c - 2)
    across(chunks - 1)
    back(chunks - 2)
    conv[0].wait_recv()
    for n in range(4):
        conv_y[n].wait_recv()
        at = pl.multiple_of(me * span + n * piece_rows, piece_rows)
        conv_out[n * piece_rows : (n + 1) * piece_rows, :] = (
            partial[pl.ds(at, piece_rows), :].astype(f32)
            + conv_core[0, n * piece_rows : (n + 1) * piece_rows, :].astype(f32)
            + conv_from_y[n].astype(f32)
        ).astype(bf16)
    back(chunks - 1)

    for r in backs:
        r.wait_recv()
    scale = jnp.concatenate(
        [jnp.where(h, weights[s : s + 1, :], 0.0) for s, h in enumerate(held)], axis=0
    ).T.astype(bf16)
    for n in range(0, width, tile):
        combined[:, n : n + tile] = jnp.dot(
            scale, returned[:, n : n + tile], preferred_element_type=f32
        ).astype(bf16)
    last = [
        remote(
            block(combined, core if n == 0 else far, rows), last_core.at[n],
            last_send.at[n], last_recv.at[n], {"tp": core},
        )
        for n in range(2)
    ]
    last[1].start()
    last[0].start()
    last.append(remote(last_to_y, last_from_y, last_send.at[2], last_recv.at[2], {"tp": over}))

    def own(quarter, n):
        at = pl.multiple_of(quarter * rows, rows)
        return combined[pl.ds(at, rows), :].astype(f32) + last_core[n].astype(f32)

    last[1].wait_recv()
    last_to_y[...] = own(over, 1).astype(bf16)
    last[2].start()
    last[0].wait_recv()
    last[2].wait_recv()
    moe_out[...] = (own(me, 0) + last_from_y[...].astype(f32)).astype(bf16)
    sent += last
    for r in sent:
        r.wait_send()


def run_exchange(
    normed, ranks, weights, mixed, stats, gain, shift, proj, gate, up, down, ep_count, share
):
    rows, width = normed.shape
    hid = gate.shape[1]
    conv_rows = mixed.shape[0]
    span = conv_rows // 4
    bf16 = jnp.bfloat16
    slots = ep_count * share
    vmem, dma = pltpu.VMEM, pltpu.SemaphoreType.DMA
    at_vmem, at_any = pl.BlockSpec(memory_space=pltpu.VMEM), pl.BlockSpec(memory_space=pl.ANY)
    return pl.pallas_call(
        functools.partial(exchange, ep_count=ep_count, share=share),
        out_shape=(
            jax.ShapeDtypeStruct((span, width), bf16),
            jax.ShapeDtypeStruct((rows, width), bf16),
        ),
        in_specs=[at_vmem] * 8 + [at_any] * 3,
        out_specs=(at_vmem, at_vmem),
        scratch_shapes=[
            vmem((conv_rows, width), bf16),
            vmem((3, 8, conv_rows), jnp.float32),
            vmem((conv_rows, 8), jnp.float32),
            vmem((width, hid), bf16),
            vmem((width, hid), bf16),
            vmem((hid, width), bf16),
            vmem((4 * rows, width), bf16),
            vmem((slots, width), bf16),
            vmem((4 * slots, width), bf16),
            vmem((4 * slots, width), bf16),
            vmem((ep_count, 2, share, width), bf16),
            vmem((ep_count, share, width), bf16),
            vmem((ep_count, share, width), bf16),
            vmem((ep_count, share, width), bf16),
            vmem((slots, width), bf16),
            vmem((2, span, width), bf16),
            vmem((4, span // 4, width), bf16),
            vmem((4, span // 4, width), bf16),
            vmem((4 * rows, width), bf16),
            vmem((2, rows, width), bf16),
            vmem((rows, width), bf16),
            vmem((rows, width), bf16),
            dma((3,)),
            dma((3,)), dma((3,)),
            dma((3,)), dma((3,)),
            dma((ep_count,)), dma((ep_count,)),
            dma((3, ep_count)), dma((3, ep_count)),
            dma((ep_count, 2)), dma((ep_count, 2)),
            dma((ep_count,)), dma((ep_count,)),
            dma((ep_count,)), dma((ep_count,)),
            dma((6,)), dma((6,)),
            dma((3,)), dma((3,)),
        ],
        compiler_params=pltpu.CompilerParams(
            collective_id=0, has_side_effects=True, vmem_limit_bytes=60 * 1024 * 1024
        ),
    )(normed, ranks, weights, mixed, stats, gain, shift, proj, gate, up, down)


def shifted(value, axis, steps):
    count = lax.axis_size(axis)
    leading, last = (max(0, -steps), min(count, count - steps))
    return lax.ppermute(value, axis, [(source, source + steps) for source in range(leading, last)])


def local(
    conv_input,
    conv_kernel,
    norm_gain,
    norm_shift,
    conv_proj,
    moe_input,
    moe_gain,
    routes,
    route_weights,
    gate_proj,
    up_proj,
    down_proj,
):
    tp_count = lax.axis_size("tp")
    ep_count = lax.axis_size("ep")
    local_rows, local_width = conv_input.shape
    reach = conv_kernel.shape[0] - 1
    history = shifted(conv_input[local_rows - reach :], "ep", 1)
    padded = jnp.concatenate([history, conv_input], axis=0)
    taps = conv_kernel.astype(jnp.float32)
    mixed = jnp.zeros((local_rows, local_width), jnp.float32)
    for offset in range(reach + 1):
        mixed = mixed + padded[offset : offset + local_rows].astype(jnp.float32) * taps[offset]
    row_sums, row_squares = jnp.sum(mixed, axis=1), jnp.sum(mixed * mixed, axis=1)
    moe_float = moe_input.astype(jnp.float32)
    normed = (
        moe_float
        * lax.rsqrt(jnp.mean(moe_float * moe_float, axis=1, keepdims=True) + 1e-06)
        * moe_gain
    ).astype(jnp.bfloat16)
    group_rows, top_count = routes.shape
    model_width = normed.shape[1]
    capacity = 2 * top_count * group_rows // ep_count
    share = capacity // tp_count
    direct = tp_count == 4 and share % 16 == 0 and ep_count % 2 == 0 and ep_count >= 8
    if direct:
        hops = jnp.array(hop_order(ep_count), jnp.int32)
        experts = (lax.axis_index("ep") + hops) % ep_count
    else:
        experts = jnp.arange(ep_count, dtype=jnp.int32)
    named = routes.T[None, :, :] == experts[:, None, None]
    hit = jnp.any(named, axis=1)
    weight = jnp.sum(jnp.where(named, route_weights.T[None, :, :], 0.0), axis=1)
    tokens = jnp.arange(group_rows, dtype=jnp.int32)
    before = (tokens[:, None] < tokens[None, :]).astype(jnp.bfloat16)
    rank = jnp.dot(hit.astype(jnp.bfloat16), before, preferred_element_type=jnp.float32).astype(
        jnp.int32
    )
    if direct:
        ranks = jnp.where(hit, rank, -1)
        idle = jnp.zeros((6, local_rows), jnp.float32)
        stats = jnp.concatenate([row_sums[None, :], row_squares[None, :], idle], axis=0)
        return run_exchange(
            normed, ranks, weight, mixed, stats, norm_gain[None, :], norm_shift[None, :],
            conv_proj, gate_proj[0], up_proj[0], down_proj[0], ep_count, share,
        )
    full_width = local_width * tp_count
    sums, squares = lax.psum((row_sums, row_squares), "tp")
    center = sums / full_width
    spread = jnp.maximum(squares / full_width - center * center, 0.0)
    scaled = (mixed - center[:, None]) * lax.rsqrt(spread[:, None] + 1e-05) * norm_gain + norm_shift
    activated = jax.nn.silu(scaled).astype(jnp.bfloat16)
    partial = jnp.dot(activated, conv_proj, preferred_element_type=jnp.float32).astype(jnp.bfloat16)
    first = lax.axis_index("tp") * share
    slots = first + jnp.arange(share, dtype=jnp.int32)
    held = hit[:, None, :] & (rank[:, None, :] == slots[None, :, None])
    pick = held.astype(jnp.bfloat16).reshape(ep_count * share, group_rows)
    scale = (
        jnp.where(held, weight[:, None, :], 0.0)
        .astype(jnp.bfloat16)
        .reshape(ep_count * share, group_rows)
    )
    conv_out = lax.psum_scatter(partial, "tp", scatter_dimension=0, tiled=True)
    group = lax.all_gather(normed, "tp", axis=0, tiled=True)
    outgoing = jnp.dot(pick, group, preferred_element_type=jnp.float32).astype(jnp.bfloat16)
    landed = lax.all_to_all(
        outgoing.reshape(ep_count, share, model_width), "ep", split_axis=0, concat_axis=0, tiled=True
    ).reshape(ep_count * share, model_width)
    incoming = lax.all_gather(landed, "tp", axis=0, tiled=True)
    gated = jax.nn.silu(jnp.dot(incoming, gate_proj[0], preferred_element_type=jnp.float32))
    hidden = (gated * jnp.dot(incoming, up_proj[0], preferred_element_type=jnp.float32)).astype(
        jnp.bfloat16
    )
    pieces = jnp.dot(hidden, down_proj[0], preferred_element_type=jnp.float32).astype(jnp.bfloat16)
    summed = lax.psum_scatter(pieces, "tp", scatter_dimension=0, tiled=True)
    returned = lax.all_to_all(
        summed.reshape(ep_count, share, model_width), "ep", split_axis=0, concat_axis=0, tiled=True
    ).reshape(ep_count * share, model_width)
    combined = lax.dot_general(
        scale, returned, (((0,), (0,)), ((), ())), preferred_element_type=jnp.float32
    )
    moe_out = lax.psum_scatter(combined.astype(jnp.bfloat16), "tp", scatter_dimension=0, tiled=True)
    return (conv_out, moe_out)


def solution(mesh):
    placed = (
        P("ep", "tp"),
        P(None, "tp"),
        P("tp"),
        P("tp"),
        P("tp", None),
        P(("ep", "tp"), None),
        P(),
        P("ep", None),
        P("ep", None),
        P("ep", None, "tp"),
        P("ep", None, "tp"),
        P("ep", "tp", None),
    )
    return jax.shard_map(
        local,
        mesh=mesh,
        in_specs=placed,
        out_specs=(P(("ep", "tp"), None), P(("ep", "tp"), None)),
        check_vma=False,
    )
```
